32 devices in a mesh: sp: 8 (over z, x), tp: 4 (over y, core).
Axes of the slice: x: 2, y: 2, z: 4, core: 2. Of those that a mesh axis runs over, the one named last changes fastest.
Arguments:
- latent: bfloat16 [4096, 4096], P('sp'), may hold values from -64 to 64
- context: bfloat16 [512, 4096], P('sp'), may hold values from -6 to 6
- condition: bfloat16 [4096], P('sp'), may hold values from -6 to 6
- context_condition: bfloat16 [4096], P('sp'), may hold values from -6 to 6
- shift_weight: bfloat16 [4096, 4096], P('sp', 'tp'), may hold values from -0.125 to 0.125
- scale_weight: bfloat16 [4096, 4096], P('sp', 'tp'), may hold values from -0.125 to 0.125
- gate_weight: bfloat16 [4096, 4096], P('sp', 'tp'), may hold values from -0.25 to 0.25
- norm_gain: float32 [4096], replicated, may hold values from 0.1 to 1.9
- query_weight: bfloat16 [4096, 2048], P(None, 'tp'), may hold values from -0.09375 to 0.09375
- key_weight: bfloat16 [4096, 2048], P(None, 'tp'), may hold values from -0.09375 to 0.09375
- value_weight: bfloat16 [4096, 2048], P(None, 'tp'), may hold values from -0.09375 to 0.09375
- write_weight: bfloat16 [4096, 2, 16], replicated, may hold values from -0.09375 to 0.09375
- decay_weight: bfloat16 [4096, 2, 16], replicated, may hold values from -0.09375 to 0.09375
- write_bias: float32 [2, 16], replicated, may hold values from -12 to 1
- decay_bias: float32 [2, 16], replicated, may hold values from -16 to -4
- log_rate: float32 [2, 16], replicated, may hold values from 0 to 1.4
- head_gain: float32 [128], replicated, may hold values from 0.1 to 1.9
- out_weight: bfloat16 [2048, 4096], P(None, 'tp'), may hold values from -0.125 to 0.125
Outputs:
- updated: bfloat16 [4096, 4096], P('sp', 'tp')
The draws below stay inside these ranges and needn't reach their ends.
All inputs are finite; a program needn't handle non-finite values.
Results may differ from the reference program's by a relative error of at most 0.013.
Values may be sent and summed in bfloat16 or wider, within the bound.
A program may use at most 128 MiB of HBM per device.

```python
import math
import jax
import jax.numpy as jnp
from jax import lax

D = 4096
HEADS = 16
HEAD_DIM = 128
BLOCK = 64
TOKENS = 4096
CTX = 512


def draw_latent(key, part):
    segment_count = (TOKENS + 127) // 128
    offsets = jnp.clip(jax.random.normal(jax.random.fold_in(key, 22), (segment_count, D), jnp.float32), -3.0, 3.0)
    segment_index = jnp.arange(TOKENS) // 128
    noise = jnp.clip(jax.random.normal(jax.random.fold_in(key, 21), (TOKENS, D), jnp.float32), -6.0, 6.0)
    return (noise + offsets[segment_index]).astype(jnp.bfloat16)


def head_speeds(key):
    chooser = jax.random.uniform(jax.random.fold_in(key, 31), (2, HEADS), jnp.float32)
    return chooser < 0.7


def draw_decay_bias(key, part):
    keeping = head_speeds(key)
    spread = jax.random.uniform(jax.random.fold_in(key, 32), (2, HEADS), jnp.float32, -0.5, 0.5)
    slow_value = math.log(0.05 / (TOKENS + CTX)) + spread
    fast_value = -5.0 + spread
    return jnp.where(keeping, slow_value, fast_value).astype(jnp.float32)


def draw_write_bias(key, part):
    keeping = head_speeds(key)
    spread = jax.random.uniform(jax.random.fold_in(key, 33), (2, HEADS), jnp.float32, -0.5, 0.5)
    slow_value = math.log(HEAD_DIM / (TOKENS + CTX)) - 1.5 + spread
    fast_value = spread
    return jnp.where(keeping, slow_value, fast_value).astype(jnp.float32)


def block_levels(rng, shape, cuts, least, high):
    level = 1.0
    for position, blocks in cuts:
        draws = jax.random.uniform(jax.random.fold_in(jax.random.fold_in(rng, 6), position), (blocks,), jnp.float32, least / len(cuts), high / len(cuts))
        level = level * jnp.repeat(jnp.exp(draws), shape[position] // blocks).reshape((-1,) + (1,) * (len(shape) - 1 - position))
    return level


def gaussian(key, extent, scale, most, split=(), held_as=jnp.bfloat16):
    drawn = jax.random.normal(key, extent, jnp.float32) * scale
    if len(split) > 0:
        drawn = block_levels(key, extent, split, -0.22, 0.18) * drawn
    return jnp.clip(drawn, min=-most, max=most).astype(held_as)


def setup_inputs(seed: int = 0) -> dict:
    keys = jax.random.split(jax.random.key(seed), 19)
    return {
        "latent": draw_latent(jax.random.fold_in(keys[18], 71), 0),
        "context": gaussian(keys[1], (CTX, D), 1.0, 6.0, ((0, 8),)),
        "condition": gaussian(keys[2], (D,), 1.0, 6.0, ((0, 8),)),
        "context_condition": gaussian(keys[3], (D,), 1.0, 6.0, ((0, 8),)),
        "shift_weight": gaussian(keys[4], (D, D), (D // 2) ** -0.5, 0.125, ((0, 8), (1, 4))),
        "scale_weight": gaussian(keys[5], (D, D), (D // 2) ** -0.5, 0.125, ((0, 8), (1, 4))),
        "gate_weight": gaussian(keys[6], (D, D), (D // 8) ** -0.5, 0.25, ((0, 8), (1, 4))),
        "norm_gain": jnp.clip(1.0 + 0.18 * jax.random.normal(keys[7], (D,), jnp.float32), 0.1, 1.9),
        "query_weight": gaussian(keys[8], (D, HEADS * HEAD_DIM), D ** -0.5, 0.09375, ((1, 4),)),
        "key_weight": gaussian(keys[9], (D, HEADS * HEAD_DIM), D ** -0.5, 0.09375, ((1, 4),)),
        "value_weight": gaussian(keys[10], (D, HEADS * HEAD_DIM), D ** -0.5, 0.09375, ((1, 4),)),
        "write_weight": gaussian(keys[11], (D, 2, HEADS), D ** -0.5, 0.09375),
        "decay_weight": gaussian(keys[12], (D, 2, HEADS), D ** -0.5, 0.09375),
        "write_bias": draw_write_bias(jax.random.fold_in(keys[18], 71), 0),
        "decay_bias": draw_decay_bias(jax.random.fold_in(keys[18], 71), 0),
        "log_rate": jnp.clip(jax.random.uniform(keys[15], (2, HEADS), jnp.float32, 0.0, 1.4), 0.0, 1.4),
        "head_gain": jnp.clip(1.0 + 0.18 * jax.random.normal(keys[16], (HEAD_DIM,), jnp.float32), 0.1, 1.9),
        "out_weight": gaussian(keys[17], (HEADS * HEAD_DIM, D), (HEADS * HEAD_DIM) ** -0.5, 0.125, ((1, 4),)),
    }


epsilon = 0.0001
highest = lax.Precision.HIGHEST

def rms_rows(row_data, row_gain):
    values = row_data.astype(jnp.float32)
    scaled = values * lax.rsqrt(lax.optimization_barrier(jnp.mean(values * values, axis=-1, keepdims=True)) + epsilon)
    return scaled * row_gain.astype(jnp.float32)

def unit_heads(matrix, head_count):
    split_heads = matrix.astype(jnp.float32).reshape(matrix.shape[0], head_count, -1)
    return split_heads * lax.rsqrt(lax.optimization_barrier(jnp.sum(split_heads * split_heads, axis=-1, keepdims=True)) + epsilon)

def head_gates(write_pre, decay_pre, write_bias, decay_bias, log_rate):
    write_rate = jax.nn.sigmoid(write_pre.astype(jnp.float32) + write_bias)
    log_decay = -jnp.exp(log_rate) * jax.nn.softplus(decay_pre.astype(jnp.float32) + decay_bias)
    return (write_rate, log_decay)

def project(matrix, weight):
    return jnp.dot(matrix.astype(jnp.float32), weight.astype(jnp.float32), preferred_element_type=jnp.float32).astype(jnp.bfloat16)

def to_blocks(source):
    heads_first = jnp.moveaxis(source, 1, 0)
    block_count = heads_first.shape[1] // BLOCK
    return heads_first.reshape((heads_first.shape[0], block_count, BLOCK) + heads_first.shape[2:])

def prepare_keys(key_vecs, value_vecs, log_decay, write_rate):
    block_keys = to_blocks(key_vecs)
    block_values = to_blocks(value_vecs)
    running = jnp.cumsum(to_blocks(log_decay), axis=-1)
    block_rates = to_blocks(write_rate)
    offsets = jnp.arange(BLOCK)
    lower_mask = offsets[:, None] >= offsets[None, :]
    strict_mask = offsets[:, None] > offsets[None, :]
    spread = running[..., :, None] - running[..., None, :]
    decay_mat = jnp.where(lower_mask, jnp.exp(jnp.where(lower_mask, spread, 0.0)), 0.0)
    scaled = block_keys * block_rates[..., None]
    system = jnp.einsum('hnid,hnjd->hnij', scaled, block_keys, precision=highest) * decay_mat
    system = jnp.where(strict_mask, system, 0.0) + jnp.eye(BLOCK, dtype=system.dtype)
    fresh_values = jax.scipy.linalg.solve_triangular(system, block_values * block_rates[..., None], lower=True, unit_diagonal=True)
    key_weights = jax.scipy.linalg.solve_triangular(system, scaled * jnp.exp(running)[..., None], lower=True, unit_diagonal=True)
    last_gate = running[..., -1]
    late_keys = block_keys * jnp.exp(last_gate[..., None] - running)[..., None]
    return (block_keys, running, decay_mat, fresh_values, key_weights, last_gate, late_keys)

def prepare_queries(query_vecs, prepared):
    block_queries = to_blocks(query_vecs)
    query_keys = jnp.einsum('hnid,hnjd->hnij', block_queries, prepared[0], precision=highest) * prepared[2]
    early_queries = block_queries * jnp.exp(prepared[1])[..., None]
    return (query_keys, early_queries)

def run_blocks(prepared, queried, start):
    inputs = tuple((jnp.moveaxis(item, 1, 0) for item in (prepared[3], prepared[4], queried[0], queried[1], prepared[6], prepared[5])))

    def advance(carried, pieces):
        new_in, key_in, score_in, query_in, late_in, gate_in = pieces
        corrected = new_in - jnp.einsum('hcd,hde->hce', key_in, carried, precision=highest)
        output = jnp.einsum('hcd,hde->hce', query_in, carried, precision=highest)
        output = output + jnp.einsum('hij,hje->hie', score_in, corrected, precision=highest)
        carried = carried * jnp.exp(gate_in)[:, None, None] + jnp.einsum('hcd,hce->hde', late_in, corrected, precision=highest)
        return (carried, output)
    closing, outputs = lax.scan(advance, start, inputs)
    merged = jnp.transpose(outputs, (0, 2, 1, 3))
    return merged.reshape(-1, merged.shape[2], merged.shape[3])

def final_state(prepared, start):
    inputs = tuple((jnp.moveaxis(item, 1, 0) for item in (prepared[3], prepared[4], prepared[6], prepared[5])))

    def advance(carried, pieces):
        new_in, key_in, late_in, gate_in = pieces
        corrected = new_in - jnp.einsum('hcd,hde->hce', key_in, carried, precision=highest)
        carried = carried * jnp.exp(gate_in)[:, None, None] + jnp.einsum('hcd,hce->hde', late_in, corrected, precision=highest)
        return (carried, None)
    closing, unused = lax.scan(advance, start, inputs)
    return closing

def reference(latent, context, condition, context_condition, shift_weight, scale_weight, gate_weight, norm_gain, query_weight, key_weight, value_weight, write_weight, decay_weight, write_bias, decay_bias, log_rate, head_gain, out_weight):
    head_count = write_bias.shape[1]
    width = write_weight.shape[0]
    stacked = jnp.stack([condition, context_condition]).astype(jnp.float32)
    silu_rows = jax.nn.silu(stacked).astype(jnp.bfloat16)
    shift_rows = jnp.dot(silu_rows.astype(jnp.float32), shift_weight.astype(jnp.float32), preferred_element_type=jnp.float32)
    scale_rows = jnp.dot(silu_rows.astype(jnp.float32), scale_weight.astype(jnp.float32), preferred_element_type=jnp.float32)
    gate_row = jnp.dot(silu_rows[0].astype(jnp.float32), gate_weight.astype(jnp.float32), preferred_element_type=jnp.float32)
    modulated = (rms_rows(latent, norm_gain) * (1.0 + scale_rows[0]) + shift_rows[0]).astype(jnp.bfloat16)
    ctx_modulated = (rms_rows(context, norm_gain) * (1.0 + scale_rows[1]) + shift_rows[1]).astype(jnp.bfloat16)
    write_flat = write_weight.reshape(width, -1)
    decay_flat = decay_weight.reshape(width, -1)
    ctx_keys = unit_heads(project(ctx_modulated, key_weight), head_count)
    ctx_values = project(ctx_modulated, value_weight).astype(jnp.float32).reshape(-1, head_count, HEAD_DIM)
    ctx_rate, ctx_log = head_gates(project(ctx_modulated, write_flat).reshape(-1, 2, head_count), project(ctx_modulated, decay_flat).reshape(-1, 2, head_count), write_bias, decay_bias, log_rate)
    start_zero = jnp.zeros((head_count, HEAD_DIM, HEAD_DIM), jnp.float32)
    ctx_forward = final_state(prepare_keys(ctx_keys, ctx_values, ctx_log[:, 0], ctx_rate[:, 0]), start_zero)
    ctx_backward = final_state(prepare_keys(jnp.flip(ctx_keys, 0), jnp.flip(ctx_values, 0), jnp.flip(ctx_log[:, 1], 0), jnp.flip(ctx_rate[:, 1], 0)), start_zero)
    queries = unit_heads(project(modulated, query_weight), head_count) * HEAD_DIM ** (-0.5)
    key_vecs = unit_heads(project(modulated, key_weight), head_count)
    value_vecs = project(modulated, value_weight).astype(jnp.float32).reshape(-1, head_count, HEAD_DIM)
    write_rate, log_decay = head_gates(project(modulated, write_flat).reshape(-1, 2, head_count), project(modulated, decay_flat).reshape(-1, 2, head_count), write_bias, decay_bias, log_rate)
    forward_prep = prepare_keys(key_vecs, value_vecs, log_decay[:, 0], write_rate[:, 0])
    forward_out = run_blocks(forward_prep, prepare_queries(queries, forward_prep), ctx_forward)
    backward_prep = prepare_keys(jnp.flip(key_vecs, 0), jnp.flip(value_vecs, 0), jnp.flip(log_decay[:, 1], 0), jnp.flip(write_rate[:, 1], 0))
    backward_out = jnp.flip(run_blocks(backward_prep, prepare_queries(jnp.flip(queries, 0), backward_prep), ctx_backward), 0)
    combined = forward_out + backward_out
    head_out = combined * lax.rsqrt(lax.optimization_barrier(jnp.mean(combined * combined, axis=-1, keepdims=True)) + epsilon) * head_gain.astype(jnp.float32)
    head_out = head_out.astype(jnp.bfloat16).reshape(combined.shape[0], -1)
    branch = jnp.dot(head_out.astype(jnp.float32), out_weight.astype(jnp.float32), preferred_element_type=jnp.float32)
    return (latent.astype(jnp.float32) + gate_row * branch).astype(jnp.bfloat16)
```

```python
import functools

import jax
import jax.numpy as jnp
from jax import lax
from jax.experimental import pallas as pl
from jax.experimental.pallas import tpu as pltpu
from jax.sharding import PartitionSpec as P

HEAD_DIM = 128
CHUNK = 128
epsilon = 0.0001
bf16 = jnp.bfloat16
f32 = jnp.float32


def mm(a, b):
    return jnp.dot(a.astype(bf16), b.astype(bf16), preferred_element_type=f32)


def spans(tokens, ctx_tokens):
    size = min(CHUNK, tokens)
    lat = [(at, size) for at in range(0, tokens, size)]
    ctx_size = min(CHUNK, ctx_tokens)
    ctx = [(tokens + at, ctx_size) for at in range(0, ctx_tokens, ctx_size)]
    return lat, ctx


def prep_kernel(tokens, ctx_tokens, q_ref, k_ref, v_ref, col_ref, row_ref, o_ref, e_ref, map_ref):
    lat, ctx = spans(tokens, ctx_tokens)
    items = []
    shared = {}
    for at, size in lat + ctx:
        keys = k_ref[at : at + size, :]
        keys_t = keys.astype(f32).T
        gram = jnp.dot(keys, keys_t.astype(bf16), preferred_element_type=f32)
        rows = lax.broadcasted_iota(jnp.int32, (size, size), 0)
        cols = lax.broadcasted_iota(jnp.int32, (size, size), 1)
        diag = jnp.where(rows == cols, gram, 0.0)
        s_col = lax.rsqrt(jnp.sum(diag, axis=1, keepdims=True) + epsilon)
        s_row = lax.rsqrt(jnp.sum(diag, axis=0, keepdims=True) + epsilon)
        gram = gram * s_col * s_row
        entry = dict(keys=keys.astype(f32) * s_col, keys_t=keys_t * s_row, values=v_ref[at : at + size, :].astype(f32))
        if at < tokens:
            queries = q_ref[at : at + size, :].astype(f32)
            q_scale = lax.rsqrt(jnp.sum(queries * queries, axis=1, keepdims=True) + epsilon) * HEAD_DIM**-0.5
            entry["queries"] = queries * q_scale
            entry["score"] = (
                jnp.dot(q_ref[at : at + size, :], keys_t.astype(bf16), preferred_element_type=f32) * q_scale * s_row
            )
        shared[at] = entry
        for d in range(2):
            rate_col = col_ref[0, at : at + size, 2 * d : 2 * d + 1]
            run_col = col_ref[0, at : at + size, 2 * d + 1 : 2 * d + 2]
            run_row = row_ref[0, 2 * d + 1 : 2 * d + 2, at : at + size]
            inside = rows >= cols if d == 0 else rows <= cols
            strict = rows > cols if d == 0 else rows < cols
            decay = jnp.where(inside, jnp.exp(jnp.minimum(run_col - run_row, 0.0)), 0.0)
            system = jnp.where(strict, gram * decay * rate_col, 0.0)
            item = dict(at=at, size=size, d=d, rate_col=rate_col, run_col=run_col, run_row=run_row)
            item["system"] = system
            if at < tokens:
                item["score"] = entry["score"] * decay
            near = (rows // 2) == (cols // 2)
            item["inv"] = jnp.where(rows == cols, 1.0, jnp.where(near, -system, 0.0))
            items.append(item)
    span = 2
    while span < max(item["size"] for item in items):
        firsts = []
        for item in items:
            if span >= item["size"]:
                firsts.append(None)
                continue
            size = item["size"]
            rows = lax.broadcasted_iota(jnp.int32, (size, size), 0) // span
            cols = lax.broadcasted_iota(jnp.int32, (size, size), 1) // span
            if item["d"] == 0:
                mask = ((rows % 2) == 1) & (cols == rows - 1)
            else:
                mask = ((cols % 2) == 1) & (rows == cols - 1)
            firsts.append(mm(jnp.where(mask, item["system"], 0.0), item["inv"]))
        for item, first in zip(items, firsts):
            if first is not None:
                item["inv"] = item["inv"] - mm(item["inv"], first)
        span *= 2
    for item in items:
        entry = shared[item["at"]]
        growth = jnp.exp(item["run_col"])
        both = jnp.concatenate(
            [entry["values"] * item["rate_col"], entry["keys"] * (item["rate_col"] * growth)], axis=1
        )
        item["solved"] = mm(item["inv"], both)
        last = item["run_row"][:, item["size"] - 1 :] if item["d"] == 0 else item["run_row"][:, :1]
        item["gate"] = jnp.exp(last)
        late_t = entry["keys_t"] * jnp.exp(last - item["run_row"])
        item["late"] = mm(late_t, item["solved"])
        if item["at"] < tokens:
            weighed = mm(item["score"], item["solved"])
            item["local"] = weighed[:, :HEAD_DIM]
            item["early"] = entry["queries"] * growth - weighed[:, HEAD_DIM:]
    eye_r = lax.broadcasted_iota(jnp.int32, (HEAD_DIM, HEAD_DIM), 0)
    eye_c = lax.broadcasted_iota(jnp.int32, (HEAD_DIM, HEAD_DIM), 1)
    eye = (eye_r == eye_c).astype(f32)

    def chain(chunks, d, emit):
        carry = None
        for item in chunks if d == 0 else chunks[::-1]:
            if emit:
                if carry is None:
                    out, early = item["local"], item["early"]
                else:
                    moved = mm(item["early"], carry)
                    out = item["local"] + moved[:, :HEAD_DIM]
                    early = item["early"] + moved[:, HEAD_DIM:]
                e_ref[0, item["at"] : item["at"] + item["size"], d * HEAD_DIM : (d + 1) * HEAD_DIM] = early.astype(
                    bf16
                )
                item["out"] = out
            late, gate = item["late"], item["gate"]
            fresh = jnp.concatenate([late[:, :HEAD_DIM], (gate - 1.0) * eye - late[:, HEAD_DIM:]], axis=1)
            if carry is None:
                carry = fresh
            else:
                carry = gate * carry + fresh - mm(late[:, HEAD_DIM:], carry)
        return carry

    for d in range(2):
        latents = [i for i in items if i["d"] == d and i["at"] < tokens]
        contexts = [i for i in items if i["d"] == d and i["at"] >= tokens]
        map_ref[0, d, 0] = chain(contexts, d, False).astype(bf16)
        map_ref[0, d, 1] = chain(latents, d, True).astype(bf16)
    for at, size in lat:
        pair = [i for i in items if i["at"] == at]
        o_ref[0, at : at + size, :] = pair[0]["out"] + pair[1]["out"]


def prepare(queries, keys, values, col, row, tokens, ctx_tokens):
    heads = col.shape[0]
    every = tokens + ctx_tokens
    return pl.pallas_call(
        functools.partial(prep_kernel, tokens, ctx_tokens),
        grid=(heads,),
        in_specs=[
            pl.BlockSpec((tokens, HEAD_DIM), lambda h: (0, h)),
            pl.BlockSpec((every, HEAD_DIM), lambda h: (0, h)),
            pl.BlockSpec((every, HEAD_DIM), lambda h: (0, h)),
            pl.BlockSpec((1, every, col.shape[2]), lambda h: (h, 0, 0)),
            pl.BlockSpec((1, row.shape[1], every), lambda h: (h, 0, 0)),
        ],
        out_specs=[
            pl.BlockSpec((1, tokens, HEAD_DIM), lambda h: (h, 0, 0)),
            pl.BlockSpec((1, tokens, 2 * HEAD_DIM), lambda h: (h, 0, 0)),
            pl.BlockSpec((1, 2, 2, HEAD_DIM, 2 * HEAD_DIM), lambda h: (h, 0, 0, 0, 0)),
        ],
        out_shape=[
            jax.ShapeDtypeStruct((heads, tokens, HEAD_DIM), f32),
            jax.ShapeDtypeStruct((heads, tokens, 2 * HEAD_DIM), bf16),
            jax.ShapeDtypeStruct((heads, 2, 2, HEAD_DIM, 2 * HEAD_DIM), bf16),
        ],
        compiler_params=pltpu.CompilerParams(vmem_limit_bytes=60 * 1024 * 1024),
        name="prepare",
    )(queries, keys, values, col, row)


def apply_maps(maps, state):
    high = state.astype(bf16)
    low = (state - high.astype(f32)).astype(bf16)
    move = maps[:, HEAD_DIM:]
    return (
        state
        + maps[:, :HEAD_DIM].astype(f32)
        + jnp.dot(move, high, preferred_element_type=f32)
        + jnp.dot(move, low, preferred_element_type=f32)
    )


def chain_kernel(peers, per, maps_ref, start_ref):
    place = lax.axis_index("sp")
    for slot in range(per):
        back = lax.rem(place * per + slot, 2)

        def at(step):
            return step + back * (peers - 1 - 2 * step)

        state = jnp.zeros((HEAD_DIM, HEAD_DIM), f32)
        for step in range(peers):
            state = apply_maps(maps_ref[at(step), slot, 0], state)
        for step in range(peers):
            start_ref[at(step), slot] = state.astype(bf16)
            if step < peers - 1:
                state = apply_maps(maps_ref[at(step), slot, 1], state)


def finish_kernel(o_ref, e_ref, s_ref, gain_ref, out_ref):
    states = s_ref[...].reshape(2 * HEAD_DIM, HEAD_DIM)
    combined = o_ref[0] + jnp.dot(e_ref[0], states, preferred_element_type=f32)
    scale = lax.rsqrt(jnp.mean(combined * combined, axis=1, keepdims=True) + epsilon)
    out_ref[...] = (combined * scale * gain_ref[...]).astype(bf16)


def finish(local, early, starts, gain):
    heads, tokens, _ = local.shape
    return pl.pallas_call(
        finish_kernel,
        grid=(heads,),
        in_specs=[
            pl.BlockSpec((1, tokens, HEAD_DIM), lambda h: (h, 0, 0)),
            pl.BlockSpec((1, tokens, 2 * HEAD_DIM), lambda h: (h, 0, 0)),
            pl.BlockSpec((2, HEAD_DIM, HEAD_DIM), lambda h: (h, 0, 0)),
            pl.BlockSpec((1, HEAD_DIM), lambda h: (0, 0)),
        ],
        out_specs=pl.BlockSpec((tokens, HEAD_DIM), lambda h: (0, h)),
        out_shape=jax.ShapeDtypeStruct((tokens, heads * HEAD_DIM), bf16),
        name="finish",
    )(local, early, starts, gain)


def start_states(maps):
    items = maps.shape[0]
    peers = lax.axis_size("sp")
    per = -(-items // peers)
    padded = jnp.pad(maps, ((0, per * peers - items), (0, 0), (0, 0), (0, 0)))
    padded = padded.reshape((peers, per) + maps.shape[1:])
    mine = lax.all_to_all(padded, "sp", 0, 0)
    starts = pl.pallas_call(
        functools.partial(chain_kernel, peers, per),
        out_shape=jax.ShapeDtypeStruct((peers, per, HEAD_DIM, HEAD_DIM), bf16),
        name="chain",
    )(mine)
    back = lax.all_to_all(starts, "sp", 0, 0)
    return back.reshape(peers * per, HEAD_DIM, HEAD_DIM)[:items]


def rms_rows(row_data, row_gain):
    values = row_data.astype(f32)
    scaled = values * lax.rsqrt(jnp.mean(values * values, axis=-1, keepdims=True) + epsilon)
    return scaled * row_gain


def project(matrix, weight):
    return jnp.dot(matrix, weight, preferred_element_type=f32).astype(bf16)


def running_sums(log_decay, size):
    parts = log_decay.reshape((-1, size) + log_decay.shape[1:])
    lower = jnp.tril(jnp.ones((size, size), f32))
    ahead = jnp.einsum("ij,njh->nih", lower, parts[:, :, 0], precision=lax.Precision.HIGHEST)
    behind = jnp.einsum("ji,njh->nih", lower, parts[:, :, 1], precision=lax.Precision.HIGHEST)
    return jnp.stack([ahead, behind], axis=2).reshape(log_decay.shape)


def body(
    latent,
    context,
    condition,
    context_condition,
    shift_weight,
    scale_weight,
    gate_weight,
    norm_gain,
    query_weight,
    key_weight,
    value_weight,
    write_weight,
    decay_weight,
    write_bias,
    decay_bias,
    log_rate,
    head_gain,
    out_weight,
):
    heads_here = query_weight.shape[1] // HEAD_DIM
    first_head = lax.axis_index("tp") * heads_here
    own_cols = gate_weight.shape[1]
    col_start = lax.axis_index("tp") * own_cols
    tokens, ctx_tokens = latent.shape[0], context.shape[0]
    stacked = jnp.stack([condition, context_condition]).astype(f32)
    silu_rows = jax.nn.silu(stacked).astype(bf16)
    partial_rows = jnp.concatenate(
        [
            jnp.dot(silu_rows, shift_weight, preferred_element_type=f32),
            jnp.dot(silu_rows, scale_weight, preferred_element_type=f32),
            jnp.dot(silu_rows[:1], gate_weight, preferred_element_type=f32),
        ],
        axis=0,
    )
    summed = jnp.sum(lax.all_gather(partial_rows, "sp"), axis=0)
    gate_row = summed[4]
    rows = lax.all_gather(summed[:4], "tp", axis=1, tiled=True)

    def modulate(row_data, row_index):
        normed = rms_rows(row_data, norm_gain)
        return (normed * (1.0 + rows[2 + row_index]) + rows[row_index]).astype(bf16)

    modulated = jnp.concatenate([modulate(latent, 0), modulate(context, 1)], axis=0)

    def own_heads(array):
        return lax.dynamic_slice_in_dim(array, first_head, heads_here, array.ndim - 1)

    gate_weights = jnp.concatenate(
        [
            own_heads(write_weight).reshape(write_weight.shape[0], -1),
            own_heads(decay_weight).reshape(decay_weight.shape[0], -1),
        ],
        axis=1,
    )
    queries = project(modulated, query_weight)
    keys = project(modulated, key_weight)
    values = project(modulated, value_weight)
    pre = project(modulated, gate_weights).astype(f32).reshape(-1, 2, 2, heads_here)
    rate = jax.nn.sigmoid(pre[:, 0] + own_heads(write_bias))
    log_decay = -jnp.exp(own_heads(log_rate)) * jax.nn.softplus(pre[:, 1] + own_heads(decay_bias))
    lat, ctx = spans(tokens, ctx_tokens)
    running = jnp.concatenate(
        [running_sums(log_decay[:tokens], lat[0][1]), running_sums(log_decay[tokens:], ctx[0][1])], axis=0
    )
    gates = jnp.stack([rate, running], axis=2)
    col = jnp.transpose(gates, (3, 0, 1, 2)).reshape(heads_here, tokens + ctx_tokens, 4)
    row = jnp.transpose(gates, (3, 1, 2, 0)).reshape(heads_here, 4, tokens + ctx_tokens)
    local, early, maps = prepare(queries, keys, values, col, row, tokens, ctx_tokens)
    starts = start_states(maps.reshape((heads_here * 2, 2) + maps.shape[3:]))
    head_out = finish(local, early, starts, head_gain[None, :])
    branch = jnp.dot(
        lax.all_gather(head_out, "tp", axis=1, tiled=True), out_weight, preferred_element_type=f32
    )
    residual = lax.dynamic_slice_in_dim(latent, col_start, own_cols, 1).astype(f32)
    return (residual + gate_row * branch).astype(bf16)


def solution(mesh):
    placed = (
        P("sp", None),
        P("sp", None),
        P("sp"),
        P("sp"),
        P("sp", "tp"),
        P("sp", "tp"),
        P("sp", "tp"),
        P(),
        P(None, "tp"),
        P(None, "tp"),
        P(None, "tp"),
        P(),
        P(),
        P(),
        P(),
        P(),
        P(),
        P(None, "tp"),
    )
    return jax.shard_map(body, mesh=mesh, in_specs=placed, out_specs=P("sp", "tp"), check_vma=False)
```

```python
import functools

import jax
import jax.numpy as jnp
from jax import lax
from jax.experimental import pallas as pl
from jax.experimental.pallas import tpu as pltpu
from jax.sharding import PartitionSpec as P

HEAD_DIM = 128
CHUNK = 128
epsilon = 0.0001
bf16 = jnp.bfloat16
f32 = jnp.float32


def mm(a, b):
    return jnp.dot(a.astype(bf16), b.astype(bf16), preferred_element_type=f32)


def spans(tokens, ctx_tokens):
    size = min(CHUNK, tokens)
    lat = [(at, size) for at in range(0, tokens, size)]
    ctx_size = min(CHUNK, ctx_tokens)
    ctx = [(tokens + at, ctx_size) for at in range(0, ctx_tokens, ctx_size)]
    return lat, ctx


def prep_kernel(tokens, ctx_tokens, q_ref, k_ref, v_ref, col_ref, row_ref, o_ref, e_ref, map_ref):
    lat, ctx = spans(tokens, ctx_tokens)
    items = []
    shared = {}
    for at, size in lat + ctx:
        keys = k_ref[at : at + size, :]
        keys_t = keys.astype(f32).T
        gram = jnp.dot(keys, keys_t.astype(bf16), preferred_element_type=f32)
        rows = lax.broadcasted_iota(jnp.int32, (size, size), 0)
        cols = lax.broadcasted_iota(jnp.int32, (size, size), 1)
        diag = jnp.where(rows == cols, gram, 0.0)
        s_col = lax.rsqrt(jnp.sum(diag, axis=1, keepdims=True) + epsilon)
        s_row = lax.rsqrt(jnp.sum(diag, axis=0, keepdims=True) + epsilon)
        gram = gram * s_col * s_row
        entry = dict(keys=keys.astype(f32) * s_col, keys_t=keys_t * s_row, values=v_ref[at : at + size, :].astype(f32))
        if at < tokens:
            queries = q_ref[at : at + size, :].astype(f32)
            q_scale = lax.rsqrt(jnp.sum(queries * queries, axis=1, keepdims=True) + epsilon) * HEAD_DIM**-0.5
            entry["queries"] = queries * q_scale
            entry["score"] = (
                jnp.dot(q_ref[at : at + size, :], keys_t.astype(bf16), preferred_element_type=f32) * q_scale * s_row
            )
        shared[at] = entry
        for d in range(2):
            rate_col = col_ref[0, at : at + size, 2 * d : 2 * d + 1]
            run_col = col_ref[0, at : at + size, 2 * d + 1 : 2 * d + 2]
            run_row = row_ref[0, 2 * d + 1 : 2 * d + 2, at : at + size]
            inside = rows >= cols if d == 0 else rows <= cols
            strict = rows > cols if d == 0 else rows < cols
            decay = jnp.where(inside, jnp.exp(jnp.minimum(run_col - run_row, 0.0)), 0.0)
            system = jnp.where(strict, gram * decay * rate_col, 0.0)
            item = dict(at=at, size=size, d=d, rate_col=rate_col, run_col=run_col, run_row=run_row)
            item["system"] = system
            if at < tokens:
                item["score"] = entry["score"] * decay
            near = (rows // 2) == (cols // 2)
            item["inv"] = jnp.where(rows == cols, 1.0, jnp.where(near, -system, 0.0))
            items.append(item)
    span = 2
    while span < max(item["size"] for item in items):
        firsts = []
        for item in items:
            if span >= item["size"]:
                firsts.append(None)
                continue
            size = item["size"]
            rows = lax.broadcasted_iota(jnp.int32, (size, size), 0) // span
            cols = lax.broadcasted_iota(jnp.int32, (size, size), 1) // span
            if item["d"] == 0:
                mask = ((rows % 2) == 1) & (cols == rows - 1)
            else:
                mask = ((cols % 2) == 1) & (rows == cols - 1)
            firsts.append(mm(jnp.where(mask, item["system"], 0.0), item["inv"]))
        for item, first in zip(items, firsts):
            if first is not None:
                item["inv"] = item["inv"] - mm(item["inv"], first)
        span *= 2
    for item in items:
        entry = shared[item["at"]]
        growth = jnp.exp(item["run_col"])
        both = jnp.concatenate(
            [entry["values"] * item["rate_col"], entry["keys"] * (item["rate_col"] * growth)], axis=1
        )
        item["solved"] = mm(item["inv"], both)
        last = item["run_row"][:, item["size"] - 1 :] if item["d"] == 0 else item["run_row"][:, :1]
        item["gate"] = jnp.exp(last)
        late_t = entry["keys_t"] * jnp.exp(last - item["run_row"])
        item["late"] = mm(late_t, item["solved"])
        if item["at"] < tokens:
            weighed = mm(item["score"], item["solved"])
            item["local"] = weighed[:, :HEAD_DIM]
            item["early"] = entry["queries"] * growth - weighed[:, HEAD_DIM:]
    eye_r = lax.broadcasted_iota(jnp.int32, (HEAD_DIM, HEAD_DIM), 0)
    eye_c = lax.broadcasted_iota(jnp.int32, (HEAD_DIM, HEAD_DIM), 1)
    eye = (eye_r == eye_c).astype(f32)

    def chain(chunks, d, emit):
        carry = None
        for item in chunks if d == 0 else chunks[::-1]:
            if emit:
                if carry is None:
                    out, early = item["local"], item["early"]
                else:
                    moved = mm(item["early"], carry)
                    out = item["local"] + moved[:, :HEAD_DIM]
                    early = item["early"] + moved[:, HEAD_DIM:]
                e_ref[0, item["at"] : item["at"] + item["size"], d * HEAD_DIM : (d + 1) * HEAD_DIM] = early.astype(
                    bf16
                )
                item["out"] = out
            late, gate = item["late"], item["gate"]
            fresh = jnp.concatenate([late[:, :HEAD_DIM], (gate - 1.0) * eye - late[:, HEAD_DIM:]], axis=1)
            if carry is None:
                carry = fresh
            else:
                carry = gate * carry + fresh - mm(late[:, HEAD_DIM:], carry)
        return carry

    for d in range(2):
        latents = [i for i in items if i["d"] == d and i["at"] < tokens]
        contexts = [i for i in items if i["d"] == d and i["at"] >= tokens]
        map_ref[0, d] = chain(contexts, d, False).astype(bf16)
        map_ref[1, d] = chain(latents, d, True).astype(bf16)
    for at, size in lat:
        pair = [i for i in items if i["at"] == at]
        o_ref[0, at : at + size, :] = pair[0]["out"] + pair[1]["out"]


def prepare(queries, keys, values, col, row, tokens, ctx_tokens):
    heads = col.shape[0]
    every = tokens + ctx_tokens
    return pl.pallas_call(
        functools.partial(prep_kernel, tokens, ctx_tokens),
        grid=(heads,),
        in_specs=[
            pl.BlockSpec((tokens, HEAD_DIM), lambda h: (0, h)),
            pl.BlockSpec((every, HEAD_DIM), lambda h: (0, h)),
            pl.BlockSpec((every, HEAD_DIM), lambda h: (0, h)),
            pl.BlockSpec((1, every, col.shape[2]), lambda h: (h, 0, 0)),
            pl.BlockSpec((1, row.shape[1], every), lambda h: (h, 0, 0)),
        ],
        out_specs=[
            pl.BlockSpec((1, tokens, HEAD_DIM), lambda h: (h, 0, 0)),
            pl.BlockSpec((1, tokens, 2 * HEAD_DIM), lambda h: (h, 0, 0)),
            pl.BlockSpec((2, 2, HEAD_DIM, 2 * HEAD_DIM), lambda h: (0, h, 0, 0)),
        ],
        out_shape=[
            jax.ShapeDtypeStruct((heads, tokens, HEAD_DIM), f32),
            jax.ShapeDtypeStruct((heads, tokens, 2 * HEAD_DIM), bf16),
            jax.ShapeDtypeStruct((2, 2 * heads, HEAD_DIM, 2 * HEAD_DIM), bf16),
        ],
        compiler_params=pltpu.CompilerParams(vmem_limit_bytes=60 * 1024 * 1024),
        name="prepare",
    )(queries, keys, values, col, row)


def apply_maps(maps, state):
    high = state.astype(bf16)
    low = (state - high.astype(f32)).astype(bf16)
    move = maps[:, HEAD_DIM:]
    return (
        state
        + maps[:, :HEAD_DIM].astype(f32)
        + jnp.dot(move, high, preferred_element_type=f32)
        + jnp.dot(move, low, preferred_element_type=f32)
    )


def on_mesh(sp=None, tp=None):
    return (lax.axis_index("sp") if sp is None else sp, lax.axis_index("tp") if tp is None else tp)


def send(src, dst, send_sem, recv_sem, device):
    return pltpu.make_async_remote_copy(
        src_ref=src,
        dst_ref=dst,
        send_sem=send_sem,
        recv_sem=recv_sem,
        device_id=device,
        device_id_type=pl.DeviceIdType.MESH,
    )


def greet(devices):
    barrier = pltpu.get_barrier_semaphore()
    for device in devices:
        pl.semaphore_signal(barrier, inc=1, device_id=device, device_id_type=pl.DeviceIdType.MESH)


def modulation_kernel(
    sp, tp, silu_ref, shift_ref, scale_ref, gate_ref, rows_ref, gate_out, got, blocks, sent_a, recv_a, sent_b, recv_b
):
    me, col = lax.axis_index("sp"), lax.axis_index("tp")
    width = shift_ref.shape[1]
    rings = [on_mesh(sp=lax.rem(me + r, sp)) for r in range(1, sp)]
    cross = [on_mesh(tp=lax.rem(col + r, tp)) for r in range(1, tp)]
    greet(rings + cross)
    silu = silu_ref[...]
    shift = jnp.dot(silu, shift_ref[...], preferred_element_type=f32)
    scale = jnp.dot(silu, scale_ref[...], preferred_element_type=f32)
    gate = jnp.dot(silu, gate_ref[...], preferred_element_type=f32)
    got[me] = jnp.concatenate([shift[0:2], scale[0:2], gate[0:1], jnp.zeros((3, width), f32)], axis=0)
    pl.semaphore_wait(pltpu.get_barrier_semaphore(), len(rings) + len(cross))
    out = []
    for r, device in enumerate(rings):
        out.append(send(got.at[me], got.at[me], sent_a.at[r], recv_a.at[me], device))
        out[-1].start()
    for r in range(1, sp):
        src = lax.rem(me + r, sp)
        send(got.at[src], got.at[src], sent_a.at[0], recv_a.at[src], on_mesh(sp=src)).wait_recv()
    total = got[0]
    for place in range(1, sp):
        total = total + got[place]
    blocks[col] = total
    gate_out[...] = total[4:5]
    for r, device in enumerate(cross):
        out.append(send(blocks.at[col], blocks.at[col], sent_b.at[r], recv_b.at[col], device))
        out[-1].start()
    for r in range(1, tp):
        src = lax.rem(col + r, tp)
        send(blocks.at[src], blocks.at[src], sent_b.at[0], recv_b.at[src], on_mesh(tp=src)).wait_recv()
    for place in range(tp):
        rows_ref[:, place * width : (place + 1) * width] = blocks[place][0:4]
    for copy in out:
        copy.wait_send()


def modulation(silu_rows, shift_weight, scale_weight, gate_weight):
    sp, tp = lax.axis_size("sp"), lax.axis_size("tp")
    width = shift_weight.shape[1]
    vmem = pl.BlockSpec(memory_space=pltpu.VMEM)
    return pl.pallas_call(
        functools.partial(modulation_kernel, sp, tp),
        in_specs=[vmem] * 4,
        out_specs=[vmem] * 2,
        out_shape=[jax.ShapeDtypeStruct((4, tp * width), f32), jax.ShapeDtypeStruct((1, width), f32)],
        scratch_shapes=[
            pltpu.VMEM((sp, 8, width), f32),
            pltpu.VMEM((tp, 8, width), f32),
            pltpu.SemaphoreType.DMA((sp,)),
            pltpu.SemaphoreType.DMA((sp,)),
            pltpu.SemaphoreType.DMA((tp,)),
            pltpu.SemaphoreType.DMA((tp,)),
        ],
        compiler_params=pltpu.CompilerParams(collective_id=0, has_side_effects=True),
        name="modulation",
    )(jnp.pad(silu_rows, ((0, 6), (0, 0))), shift_weight, scale_weight, gate_weight)


def exchange_kernel(
    sp, per, maps_ref, o_ref, e_ref, gain_ref, out_ref, got, starts, back, sent_a, recv_a, sent_b, recv_b
):
    me = lax.axis_index("sp")
    peers = [lax.rem(me + r, sp) for r in range(1, sp)]
    greet([on_mesh(sp=peer) for peer in peers])
    pl.semaphore_wait(pltpu.get_barrier_semaphore(), sp - 1)
    out = []
    for part in range(2):
        for r, peer in enumerate(peers):
            out.append(
                send(
                    maps_ref.at[part, peer],
                    got.at[part, me],
                    sent_a.at[part, r],
                    recv_a.at[part, me],
                    on_mesh(sp=peer),
                )
            )
            out[-1].start()
    got[:, me] = maps_ref[:, me]

    def arrive(part):
        for peer in peers:
            send(
                got.at[part, peer], got.at[part, peer], sent_a.at[part, 0], recv_a.at[part, peer], on_mesh(sp=peer)
            ).wait_recv()

    def at(step, slot):
        reverse = lax.rem(me * per + slot, 2)
        return step + reverse * (sp - 1 - 2 * step)

    arrive(0)
    states = [jnp.zeros((HEAD_DIM, HEAD_DIM), f32) for slot in range(per)]
    for step in range(sp):
        for slot in range(per):
            states[slot] = apply_maps(got[0, at(step, slot), slot], states[slot])
    arrive(1)
    for step in range(sp):
        for slot in range(per):
            place = at(step, slot)
            starts[place, slot] = states[slot].astype(bf16)

            @pl.when(place != me)
            def _():
                send(
                    starts.at[place, slot],
                    back.at[me, slot],
                    sent_b.at[place, slot],
                    recv_b.at[me, slot],
                    on_mesh(sp=place),
                ).start()

            if step < sp - 1:
                states[slot] = apply_maps(got[1, place, slot], states[slot])
    back[me] = starts[me]
    for peer in peers:
        for slot in range(per):
            send(
                back.at[peer, slot], back.at[peer, slot], sent_b.at[peer, slot], recv_b.at[peer, slot], on_mesh(sp=peer)
            ).wait_recv()
    for head in range(o_ref.shape[0]):
        pair = [back[item // per, item % per] for item in (2 * head, 2 * head + 1)]
        combined = o_ref[head] + jnp.dot(
            e_ref[head], jnp.concatenate(pair, axis=0), preferred_element_type=f32
        )
        scale = lax.rsqrt(jnp.mean(combined * combined, axis=1, keepdims=True) + epsilon)
        out_ref[:, head * HEAD_DIM : (head + 1) * HEAD_DIM] = (combined * scale * gain_ref[...]).astype(bf16)
    for copy in out:
        copy.wait_send()
    for peer in peers:
        for slot in range(per):
            send(
                starts.at[peer, slot],
                back.at[me, slot],
                sent_b.at[peer, slot],
                recv_b.at[me, slot],
                on_mesh(sp=peer),
            ).wait_send()


def exchange(maps, local, early, gain):
    heads, tokens, _ = local.shape
    items = maps.shape[1]
    sp = lax.axis_size("sp")
    per = -(-items // sp)
    padded = jnp.pad(maps, ((0, 0), (0, per * sp - items), (0, 0), (0, 0)))
    padded = padded.reshape((2, sp, per) + maps.shape[2:])
    vmem = pl.BlockSpec(memory_space=pltpu.VMEM)
    return pl.pallas_call(
        functools.partial(exchange_kernel, sp, per),
        in_specs=[vmem] * 4,
        out_specs=vmem,
        out_shape=jax.ShapeDtypeStruct((tokens, heads * HEAD_DIM), bf16),
        scratch_shapes=[
            pltpu.VMEM(padded.shape, bf16),
            pltpu.VMEM((sp, per, HEAD_DIM, HEAD_DIM), bf16),
            pltpu.VMEM((sp, per, HEAD_DIM, HEAD_DIM), bf16),
            pltpu.SemaphoreType.DMA((2, sp)),
            pltpu.SemaphoreType.DMA((2, sp)),
            pltpu.SemaphoreType.DMA((sp, per)),
            pltpu.SemaphoreType.DMA((sp, per)),
        ],
        compiler_params=pltpu.CompilerParams(
            collective_id=1, has_side_effects=True, vmem_limit_bytes=48 * 1024 * 1024
        ),
        name="exchange",
    )(padded, local, early, gain)


def rms_rows(row_data, row_gain):
    values = row_data.astype(f32)
    scaled = values * lax.rsqrt(jnp.mean(values * values, axis=-1, keepdims=True) + epsilon)
    return scaled * row_gain


def project(matrix, weight):
    return jnp.dot(matrix, weight, preferred_element_type=f32).astype(bf16)


def running_sums(log_decay, size):
    parts = log_decay.reshape((-1, size) + log_decay.shape[1:])
    lower = jnp.tril(jnp.ones((size, size), f32))
    ahead = jnp.einsum("ij,njh->nih", lower, parts[:, :, 0], precision=lax.Precision.HIGHEST)
    behind = jnp.einsum("ji,njh->nih", lower, parts[:, :, 1], precision=lax.Precision.HIGHEST)
    return jnp.stack([ahead, behind], axis=2).reshape(log_decay.shape)


def body(
    latent,
    context,
    condition,
    context_condition,
    shift_weight,
    scale_weight,
    gate_weight,
    norm_gain,
    query_weight,
    key_weight,
    value_weight,
    write_weight,
    decay_weight,
    write_bias,
    decay_bias,
    log_rate,
    head_gain,
    out_weight,
):
    heads_here = query_weight.shape[1] // HEAD_DIM
    first_head = lax.axis_index("tp") * heads_here
    own_cols = gate_weight.shape[1]
    col_start = lax.axis_index("tp") * own_cols
    tokens, ctx_tokens = latent.shape[0], context.shape[0]
    stacked = jnp.stack([condition, context_condition]).astype(f32)
    silu_rows = jax.nn.silu(stacked).astype(bf16)
    rows, gate_row = modulation(silu_rows, shift_weight, scale_weight, gate_weight)

    def modulate(row_data, row_index):
        normed = rms_rows(row_data, norm_gain)
        return (normed * (1.0 + rows[2 + row_index]) + rows[row_index]).astype(bf16)

    modulated = jnp.concatenate([modulate(latent, 0), modulate(context, 1)], axis=0)

    def own_heads(array):
        return lax.dynamic_slice_in_dim(array, first_head, heads_here, array.ndim - 1)

    gate_weights = jnp.concatenate(
        [
            own_heads(write_weight).reshape(write_weight.shape[0], -1),
            own_heads(decay_weight).reshape(decay_weight.shape[0], -1),
        ],
        axis=1,
    )
    queries = project(modulated, query_weight)
    keys = project(modulated, key_weight)
    values = project(modulated, value_weight)
    pre = project(modulated, gate_weights).astype(f32).reshape(-1, 2, 2, heads_here)
    rate = jax.nn.sigmoid(pre[:, 0] + own_heads(write_bias))
    log_decay = -jnp.exp(own_heads(log_rate)) * jax.nn.softplus(pre[:, 1] + own_heads(decay_bias))
    lat, ctx = spans(tokens, ctx_tokens)
    running = jnp.concatenate(
        [running_sums(log_decay[:tokens], lat[0][1]), running_sums(log_decay[tokens:], ctx[0][1])], axis=0
    )
    gates = jnp.stack([rate, running], axis=2)
    col = jnp.transpose(gates, (3, 0, 1, 2)).reshape(heads_here, tokens + ctx_tokens, 4)
    row = jnp.transpose(gates, (3, 1, 2, 0)).reshape(heads_here, 4, tokens + ctx_tokens)
    local, early, maps = prepare(queries, keys, values, col, row, tokens, ctx_tokens)
    head_out = exchange(maps, local, early, head_gain[None, :])
    branch = jnp.dot(
        lax.all_gather(head_out, "tp", axis=1, tiled=True), out_weight, preferred_element_type=f32
    )
    residual = lax.dynamic_slice_in_dim(latent, col_start, own_cols, 1).astype(f32)
    return (residual + gate_row * branch).astype(bf16)


def solution(mesh):
    placed = (
        P("sp", None),
        P("sp", None),
        P("sp"),
        P("sp"),
        P("sp", "tp"),
        P("sp", "tp"),
        P("sp", "tp"),
        P(),
        P(None, "tp"),
        P(None, "tp"),
        P(None, "tp"),
        P(),
        P(),
        P(),
        P(),
        P(),
        P(),
        P(None, "tp"),
    )
    return jax.shard_map(body, mesh=mesh, in_specs=placed, out_specs=P("sp", "tp"), check_vma=False)
```

```python
import functools

import jax
import jax.numpy as jnp
from jax import lax
from jax.experimental import pallas as pl
from jax.experimental.pallas import tpu as pltpu
from jax.sharding import PartitionSpec as P

HEAD_DIM = 128
CHUNK = 128
epsilon = 0.0001
bf16 = jnp.bfloat16
f32 = jnp.float32


def mm(a, b):
    return jnp.dot(a.astype(bf16), b.astype(bf16), preferred_element_type=f32)


def spans(tokens, ctx_tokens):
    size = min(CHUNK, tokens)
    lat = [(at, size) for at in range(0, tokens, size)]
    ctx_size = min(CHUNK, ctx_tokens)
    ctx = [(tokens + at, ctx_size) for at in range(0, ctx_tokens, ctx_size)]
    return lat, ctx


def prep_kernel(tokens, ctx_tokens, q_ref, k_ref, v_ref, col_ref, row_ref, o_ref, e_ref, map_ref):
    lat, ctx = spans(tokens, ctx_tokens)
    items = []
    shared = {}
    for at, size in lat + ctx:
        keys = k_ref[at : at + size, :]
        keys_t = keys.astype(f32).T
        gram = jnp.dot(keys, keys_t.astype(bf16), preferred_element_type=f32)
        rows = lax.broadcasted_iota(jnp.int32, (size, size), 0)
        cols = lax.broadcasted_iota(jnp.int32, (size, size), 1)
        diag = jnp.where(rows == cols, gram, 0.0)
        s_col = lax.rsqrt(jnp.sum(diag, axis=1, keepdims=True) + epsilon)
        s_row = lax.rsqrt(jnp.sum(diag, axis=0, keepdims=True) + epsilon)
        gram = gram * s_col * s_row
        entry = dict(keys=keys.astype(f32) * s_col, keys_t=keys_t * s_row, values=v_ref[at : at + size, :].astype(f32))
        if at < tokens:
            queries = q_ref[at : at + size, :].astype(f32)
            q_scale = lax.rsqrt(jnp.sum(queries * queries, axis=1, keepdims=True) + epsilon) * HEAD_DIM**-0.5
            entry["queries"] = queries * q_scale
            entry["score"] = (
                jnp.dot(q_ref[at : at + size, :], keys_t.astype(bf16), preferred_element_type=f32) * q_scale * s_row
            )
        shared[at] = entry
        for d in range(2):
            rate_col = col_ref[0, at : at + size, 2 * d : 2 * d + 1]
            run_col = col_ref[0, at : at + size, 2 * d + 1 : 2 * d + 2]
            run_row = row_ref[0, 2 * d + 1 : 2 * d + 2, at : at + size]
            inside = rows >= cols if d == 0 else rows <= cols
            strict = rows > cols if d == 0 else rows < cols
            decay = jnp.where(inside, jnp.exp(jnp.minimum(run_col - run_row, 0.0)), 0.0)
            system = jnp.where(strict, gram * decay * rate_col, 0.0)
            item = dict(at=at, size=size, d=d, rate_col=rate_col, run_col=run_col, run_row=run_row)
            item["system"] = system
            if at < tokens:
                item["score"] = entry["score"] * decay
            near = (rows // 2) == (cols // 2)
            item["inv"] = jnp.where(rows == cols, 1.0, jnp.where(near, -system, 0.0))
            items.append(item)
    span = 2
    while span < max(item["size"] for item in items):
        firsts = []
        for item in items:
            if span >= item["size"]:
                firsts.append(None)
                continue
            size = item["size"]
            rows = lax.broadcasted_iota(jnp.int32, (size, size), 0) // span
            cols = lax.broadcasted_iota(jnp.int32, (size, size), 1) // span
            if item["d"] == 0:
                mask = ((rows % 2) == 1) & (cols == rows - 1)
            else:
                mask = ((cols % 2) == 1) & (rows == cols - 1)
            firsts.append(mm(jnp.where(mask, item["system"], 0.0), item["inv"]))
        for item, first in zip(items, firsts):
            if first is not None:
                item["inv"] = item["inv"] - mm(item["inv"], first)
        span *= 2
    for item in items:
        entry = shared[item["at"]]
        growth = jnp.exp(item["run_col"])
        both = jnp.concatenate(
            [entry["values"] * item["rate_col"], entry["keys"] * (item["rate_col"] * growth)], axis=1
        )
        item["solved"] = mm(item["inv"], both)
        last = item["run_row"][:, item["size"] - 1 :] if item["d"] == 0 else item["run_row"][:, :1]
        item["gate"] = jnp.exp(last)
        late_t = entry["keys_t"] * jnp.exp(last - item["run_row"])
        item["late"] = mm(late_t, item["solved"])
        if item["at"] < tokens:
            weighed = mm(item["score"], item["solved"])
            item["local"] = weighed[:, :HEAD_DIM]
            item["early"] = entry["queries"] * growth - weighed[:, HEAD_DIM:]
    eye_r = lax.broadcasted_iota(jnp.int32, (HEAD_DIM, HEAD_DIM), 0)
    eye_c = lax.broadcasted_iota(jnp.int32, (HEAD_DIM, HEAD_DIM), 1)
    eye = (eye_r == eye_c).astype(f32)

    def chain(chunks, d, emit):
        carry = None
        for item in chunks if d == 0 else chunks[::-1]:
            if emit:
                if carry is None:
                    out, early = item["local"], item["early"]
                else:
                    moved = mm(item["early"], carry)
                    out = item["local"] + moved[:, :HEAD_DIM]
                    early = item["early"] + moved[:, HEAD_DIM:]
                e_ref[0, item["at"] : item["at"] + item["size"], d * HEAD_DIM : (d + 1) * HEAD_DIM] = early.astype(
                    bf16
                )
                item["out"] = out
            late, gate = item["late"], item["gate"]
            fresh = jnp.concatenate([late[:, :HEAD_DIM], (gate - 1.0) * eye - late[:, HEAD_DIM:]], axis=1)
            if carry is None:
                carry = fresh
            else:
                carry = gate * carry + fresh - mm(late[:, HEAD_DIM:], carry)
        return carry

    for d in range(2):
        latents = [i for i in items if i["d"] == d and i["at"] < tokens]
        contexts = [i for i in items if i["d"] == d and i["at"] >= tokens]
        map_ref[0, d] = chain(contexts, d, False).astype(bf16)
        map_ref[1, d] = chain(latents, d, True).astype(bf16)
    for at, size in lat:
        pair = [i for i in items if i["at"] == at]
        o_ref[0, at : at + size, :] = pair[0]["out"] + pair[1]["out"]


def prepare(queries, keys, values, col, row, tokens, ctx_tokens):
    heads = col.shape[0]
    every = tokens + ctx_tokens
    return pl.pallas_call(
        functools.partial(prep_kernel, tokens, ctx_tokens),
        grid=(heads,),
        in_specs=[
            pl.BlockSpec((tokens, HEAD_DIM), lambda h: (0, h)),
            pl.BlockSpec((every, HEAD_DIM), lambda h: (0, h)),
            pl.BlockSpec((every, HEAD_DIM), lambda h: (0, h)),
            pl.BlockSpec((1, every, col.shape[2]), lambda h: (h, 0, 0)),
            pl.BlockSpec((1, row.shape[1], every), lambda h: (h, 0, 0)),
        ],
        out_specs=[
            pl.BlockSpec((1, tokens, HEAD_DIM), lambda h: (h, 0, 0)),
            pl.BlockSpec((1, tokens, 2 * HEAD_DIM), lambda h: (h, 0, 0)),
            pl.BlockSpec((2, 2, HEAD_DIM, 2 * HEAD_DIM), lambda h: (0, h, 0, 0)),
        ],
        out_shape=[
            jax.ShapeDtypeStruct((heads, tokens, HEAD_DIM), f32),
            jax.ShapeDtypeStruct((heads, tokens, 2 * HEAD_DIM), bf16),
            jax.ShapeDtypeStruct((2, 2 * heads, HEAD_DIM, 2 * HEAD_DIM), bf16),
        ],
        compiler_params=pltpu.CompilerParams(vmem_limit_bytes=60 * 1024 * 1024),
        name="prepare",
    )(queries, keys, values, col, row)


def apply_maps(maps, state):
    high = state.astype(bf16)
    low = (state - high.astype(f32)).astype(bf16)
    move = maps[:, HEAD_DIM:]
    return (
        state
        + maps[:, :HEAD_DIM].astype(f32)
        + jnp.dot(move, high, preferred_element_type=f32)
        + jnp.dot(move, low, preferred_element_type=f32)
    )


def on_mesh(sp=None, tp=None):
    return (lax.axis_index("sp") if sp is None else sp, lax.axis_index("tp") if tp is None else tp)


def send(src, dst, send_sem, recv_sem, device):
    return pltpu.make_async_remote_copy(
        src_ref=src,
        dst_ref=dst,
        send_sem=send_sem,
        recv_sem=recv_sem,
        device_id=device,
        device_id_type=pl.DeviceIdType.MESH,
    )


def greet(devices):
    barrier = pltpu.get_barrier_semaphore()
    for device in devices:
        pl.semaphore_signal(barrier, inc=1, device_id=device, device_id_type=pl.DeviceIdType.MESH)


def modulation_kernel(
    sp, tp, silu_ref, shift_ref, scale_ref, gate_ref, rows_ref, gate_out, got, blocks, sent_a, recv_a, sent_b, recv_b
):
    me, col = lax.axis_index("sp"), lax.axis_index("tp")
    width = shift_ref.shape[1]
    rings = [on_mesh(sp=lax.rem(me + r, sp)) for r in range(1, sp)]
    cross = [on_mesh(tp=lax.rem(col + r, tp)) for r in range(1, tp)]
    greet(rings + cross)
    silu = silu_ref[...]
    shift = jnp.dot(silu, shift_ref[...], preferred_element_type=f32)
    scale = jnp.dot(silu, scale_ref[...], preferred_element_type=f32)
    gate = jnp.dot(silu, gate_ref[...], preferred_element_type=f32)
    got[me] = jnp.concatenate([shift[0:2], scale[0:2], gate[0:1], jnp.zeros((3, width), f32)], axis=0)
    pl.semaphore_wait(pltpu.get_barrier_semaphore(), len(rings) + len(cross))
    out = []
    for r, device in enumerate(rings):
        out.append(send(got.at[me], got.at[me], sent_a.at[r], recv_a.at[me], device))
        out[-1].start()
    for r in range(1, sp):
        src = lax.rem(me + r, sp)
        send(got.at[src], got.at[src], sent_a.at[0], recv_a.at[src], on_mesh(sp=src)).wait_recv()
    total = got[0]
    for place in range(1, sp):
        total = total + got[place]
    blocks[col] = total
    gate_out[...] = total[4:5]
    for r, device in enumerate(cross):
        out.append(send(blocks.at[col], blocks.at[col], sent_b.at[r], recv_b.at[col], device))
        out[-1].start()
    for r in range(1, tp):
        src = lax.rem(col + r, tp)
        send(blocks.at[src], blocks.at[src], sent_b.at[0], recv_b.at[src], on_mesh(tp=src)).wait_recv()
    for place in range(tp):
        rows_ref[:, place * width : (place + 1) * width] = blocks[place][0:4]
    for copy in out:
        copy.wait_send()


def modulation(silu_rows, shift_weight, scale_weight, gate_weight):
    sp, tp = lax.axis_size("sp"), lax.axis_size("tp")
    width = shift_weight.shape[1]
    vmem = pl.BlockSpec(memory_space=pltpu.VMEM)
    return pl.pallas_call(
        functools.partial(modulation_kernel, sp, tp),
        in_specs=[vmem] * 4,
        out_specs=[vmem] * 2,
        out_shape=[jax.ShapeDtypeStruct((4, tp * width), f32), jax.ShapeDtypeStruct((1, width), f32)],
        scratch_shapes=[
            pltpu.VMEM((sp, 8, width), f32),
            pltpu.VMEM((tp, 8, width), f32),
            pltpu.SemaphoreType.DMA((sp,)),
            pltpu.SemaphoreType.DMA((sp,)),
            pltpu.SemaphoreType.DMA((tp,)),
            pltpu.SemaphoreType.DMA((tp,)),
        ],
        compiler_params=pltpu.CompilerParams(collective_id=0, has_side_effects=True),
        name="modulation",
    )(jnp.pad(silu_rows, ((0, 6), (0, 0))), shift_weight, scale_weight, gate_weight)


def exchange_kernel(
    sp, per, maps_ref, o_ref, e_ref, gain_ref, out_ref, got, starts, back, sent_a, recv_a, sent_b, recv_b
):
    me = lax.axis_index("sp")
    peers = [lax.rem(me + r, sp) for r in range(1, sp)]
    greet([on_mesh(sp=peer) for peer in peers])
    pl.semaphore_wait(pltpu.get_barrier_semaphore(), sp - 1)
    out = []
    for part in range(2):
        for r, peer in enumerate(peers):
            out.append(
                send(
                    maps_ref.at[part, peer],
                    got.at[part, me],
                    sent_a.at[part, r],
                    recv_a.at[part, me],
                    on_mesh(sp=peer),
                )
            )
            out[-1].start()
    got[:, me] = maps_ref[:, me]

    def arrive(part):
        for peer in peers:
            send(
                got.at[part, peer], got.at[part, peer], sent_a.at[part, 0], recv_a.at[part, peer], on_mesh(sp=peer)
            ).wait_recv()

    def at(step, slot):
        reverse = lax.rem(me * per + slot, 2)
        return step + reverse * (sp - 1 - 2 * step)

    arrive(0)
    states = [jnp.zeros((HEAD_DIM, HEAD_DIM), f32) for slot in range(per)]
    for step in range(sp):
        for slot in range(per):
            states[slot] = apply_maps(got[0, at(step, slot), slot], states[slot])
    arrive(1)
    for step in range(sp):
        for slot in range(per):
            place = at(step, slot)
            starts[place, slot] = states[slot].astype(bf16)

            @pl.when(place != me)
            def _():
                send(
                    starts.at[place, slot],
                    back.at[me, slot],
                    sent_b.at[place, slot],
                    recv_b.at[me, slot],
                    on_mesh(sp=place),
                ).start()

            if step < sp - 1:
                states[slot] = apply_maps(got[1, place, slot], states[slot])
    back[me] = starts[me]
    for peer in peers:
        for slot in range(per):
            send(
                back.at[peer, slot], back.at[peer, slot], sent_b.at[peer, slot], recv_b.at[peer, slot], on_mesh(sp=peer)
            ).wait_recv()
    for head in range(o_ref.shape[0]):
        pair = [back[item // per, item % per] for item in (2 * head, 2 * head + 1)]
        combined = o_ref[head] + jnp.dot(
            e_ref[head], jnp.concatenate(pair, axis=0), preferred_element_type=f32
        )
        scale = lax.rsqrt(jnp.mean(combined * combined, axis=1, keepdims=True) + epsilon)
        out_ref[:, head * HEAD_DIM : (head + 1) * HEAD_DIM] = (combined * scale * gain_ref[...]).astype(bf16)
    for copy in out:
        copy.wait_send()
    for peer in peers:
        for slot in range(per):
            send(
                starts.at[peer, slot],
                back.at[me, slot],
                sent_b.at[peer, slot],
                recv_b.at[me, slot],
                on_mesh(sp=peer),
            ).wait_send()


def exchange(maps, local, early, gain):
    heads, tokens, _ = local.shape
    items = maps.shape[1]
    sp = lax.axis_size("sp")
    per = -(-items // sp)
    padded = jnp.pad(maps, ((0, 0), (0, per * sp - items), (0, 0), (0, 0)))
    padded = padded.reshape((2, sp, per) + maps.shape[2:])
    vmem = pl.BlockSpec(memory_space=pltpu.VMEM)
    return pl.pallas_call(
        functools.partial(exchange_kernel, sp, per),
        in_specs=[vmem] * 4,
        out_specs=vmem,
        out_shape=jax.ShapeDtypeStruct((tokens, heads * HEAD_DIM), bf16),
        scratch_shapes=[
            pltpu.VMEM(padded.shape, bf16),
            pltpu.VMEM((sp, per, HEAD_DIM, HEAD_DIM), bf16),
            pltpu.VMEM((sp, per, HEAD_DIM, HEAD_DIM), bf16),
            pltpu.SemaphoreType.DMA((2, sp)),
            pltpu.SemaphoreType.DMA((2, sp)),
            pltpu.SemaphoreType.DMA((sp, per)),
            pltpu.SemaphoreType.DMA((sp, per)),
        ],
        compiler_params=pltpu.CompilerParams(
            collective_id=1, has_side_effects=True, vmem_limit_bytes=48 * 1024 * 1024
        ),
        name="exchange",
    )(padded, local, early, gain)


def output_kernel(
    tp, pieces, head_ref, gate_ref, latent_ref, weight_ref, out_ref,
    got, weight, residual, acc, local_sems, sent_y, recv_y, sent_c, recv_c, sent_r, recv_r,
):
    me, col = lax.axis_index("sp"), lax.axis_index("tp")
    core = lax.rem(col, 2)
    partner = col + 1 - 2 * core
    chips = tp // 2
    far = [lax.rem(col + 2 * r, tp) for r in range(1, chips)]
    far_partner = [place + 1 - 2 * core for place in far]
    tokens, depth = head_ref.shape
    width = out_ref.shape[1]
    rows = tokens // pieces
    load = pltpu.make_async_copy(weight_ref, weight, local_sems.at[0])
    load.start()
    take = pltpu.make_async_copy(
        latent_ref.at[:, pl.ds(pl.multiple_of(col * width, width), width)], residual, local_sems.at[1]
    )
    take.start()
    greet([on_mesh(tp=place) for place in [partner] + far])
    pl.semaphore_wait(pltpu.get_barrier_semaphore(), chips)
    out = []

    def piece(ref, p):
        return ref.at[pl.ds(p * rows, rows)]

    for p in range(pieces):
        for r, place in enumerate(far):
            out.append(
                send(piece(head_ref, p), piece(got.at[col], p), sent_y.at[r, p], recv_y.at[col, p], on_mesh(tp=place))
            )
            out[-1].start()
    for p in range(pieces):
        out.append(
            send(piece(head_ref, p), piece(got.at[col], p), sent_c.at[p], recv_c.at[p], on_mesh(tp=partner))
        )
        out[-1].start()
    load.wait()

    def weights(src):
        return weight[pl.ds(pl.multiple_of(src * depth, depth), depth), :]

    def add(p, block, src, first=False):
        part = jnp.dot(block, weights(src), preferred_element_type=f32)
        at = pl.ds(p * rows, rows)
        acc[at, :] = part if first else acc[at, :] + part

    for p in range(pieces):
        add(p, head_ref[pl.ds(p * rows, rows), :], col, True)
    for p in range(pieces):
        spot = piece(got.at[partner], p)
        send(spot, spot, sent_c.at[p], recv_c.at[p], on_mesh(tp=partner)).wait_recv()
        add(p, spot[...], partner)
    take.wait()
    for p in range(pieces):
        for r, src in enumerate(far):
            spot = piece(got.at[src], p)
            send(spot, spot, sent_y.at[r, p], recv_y.at[src, p], on_mesh(tp=src)).wait_recv()
            out.append(send(spot, spot, sent_r.at[r, p], recv_r.at[src, p], on_mesh(tp=partner)))
            out[-1].start()
            add(p, spot[...], src)
        for r, src in enumerate(far_partner):
            spot = piece(got.at[src], p)
            send(spot, spot, sent_r.at[r, p], recv_r.at[src, p], on_mesh(tp=partner)).wait_recv()
            add(p, spot[...], src)
        at = pl.ds(p * rows, rows)
        out_ref[at, :] = (residual[at, :].astype(f32) + gate_ref[...] * acc[at, :]).astype(bf16)
    for copy in out:
        copy.wait_send()


def output(head_out, gate_row, latent, out_weight):
    tp = lax.axis_size("tp")
    tokens, depth = head_out.shape
    width = out_weight.shape[1]
    pieces = 4
    vmem = pl.BlockSpec(memory_space=pltpu.VMEM)
    anywhere = pl.BlockSpec(memory_space=pl.ANY)
    dma = pltpu.SemaphoreType.DMA
    return pl.pallas_call(
        functools.partial(output_kernel, tp, pieces),
        in_specs=[vmem, vmem, anywhere, anywhere],
        out_specs=vmem,
        out_shape=jax.ShapeDtypeStruct((tokens, width), bf16),
        scratch_shapes=[
            pltpu.VMEM((tp, tokens, depth), bf16),
            pltpu.VMEM(out_weight.shape, bf16),
            pltpu.VMEM((tokens, width), bf16),
            pltpu.VMEM((tokens, width), f32),
            dma((2,)),
            dma((tp, pieces)),
            dma((tp, pieces)),
            dma((pieces,)),
            dma((pieces,)),
            dma((tp, pieces)),
            dma((tp, pieces)),
        ],
        compiler_params=pltpu.CompilerParams(
            collective_id=2, has_side_effects=True, vmem_limit_bytes=48 * 1024 * 1024
        ),
        name="output",
    )(head_out, gate_row, latent, out_weight)


def rms_rows(row_data, row_gain):
    values = row_data.astype(f32)
    scaled = values * lax.rsqrt(jnp.mean(values * values, axis=-1, keepdims=True) + epsilon)
    return scaled * row_gain


def project(matrix, weight):
    return jnp.dot(matrix, weight, preferred_element_type=f32).astype(bf16)


def running_sums(log_decay, size):
    parts = log_decay.reshape((-1, size) + log_decay.shape[1:])
    lower = jnp.tril(jnp.ones((size, size), f32))
    ahead = jnp.einsum("ij,njh->nih", lower, parts[:, :, 0], precision=lax.Precision.HIGHEST)
    behind = jnp.einsum("ji,njh->nih", lower, parts[:, :, 1], precision=lax.Precision.HIGHEST)
    return jnp.stack([ahead, behind], axis=2).reshape(log_decay.shape)


def body(
    latent,
    context,
    condition,
    context_condition,
    shift_weight,
    scale_weight,
    gate_weight,
    norm_gain,
    query_weight,
    key_weight,
    value_weight,
    write_weight,
    decay_weight,
    write_bias,
    decay_bias,
    log_rate,
    head_gain,
    out_weight,
):
    heads_here = query_weight.shape[1] // HEAD_DIM
    first_head = lax.axis_index("tp") * heads_here
    tokens, ctx_tokens = latent.shape[0], context.shape[0]
    stacked = jnp.stack([condition, context_condition]).astype(f32)
    silu_rows = jax.nn.silu(stacked).astype(bf16)
    rows, gate_row = modulation(silu_rows, shift_weight, scale_weight, gate_weight)

    def modulate(row_data, row_index):
        normed = rms_rows(row_data, norm_gain)
        return (normed * (1.0 + rows[2 + row_index]) + rows[row_index]).astype(bf16)

    modulated = jnp.concatenate([modulate(latent, 0), modulate(context, 1)], axis=0)

    def own_heads(array):
        return lax.dynamic_slice_in_dim(array, first_head, heads_here, array.ndim - 1)

    gate_weights = jnp.concatenate(
        [
            own_heads(write_weight).reshape(write_weight.shape[0], -1),
            own_heads(decay_weight).reshape(decay_weight.shape[0], -1),
        ],
        axis=1,
    )
    queries = project(modulated, query_weight)
    keys = project(modulated, key_weight)
    values = project(modulated, value_weight)
    pre = project(modulated, gate_weights).astype(f32).reshape(-1, 2, 2, heads_here)
    rate = jax.nn.sigmoid(pre[:, 0] + own_heads(write_bias))
    log_decay = -jnp.exp(own_heads(log_rate)) * jax.nn.softplus(pre[:, 1] + own_heads(decay_bias))
    lat, ctx = spans(tokens, ctx_tokens)
    running = jnp.concatenate(
        [running_sums(log_decay[:tokens], lat[0][1]), running_sums(log_decay[tokens:], ctx[0][1])], axis=0
    )
    gates = jnp.stack([rate, running], axis=2)
    col = jnp.transpose(gates, (3, 0, 1, 2)).reshape(heads_here, tokens + ctx_tokens, 4)
    row = jnp.transpose(gates, (3, 1, 2, 0)).reshape(heads_here, 4, tokens + ctx_tokens)
    local, early, maps = prepare(queries, keys, values, col, row, tokens, ctx_tokens)
    head_out = exchange(maps, local, early, head_gain[None, :])
    return output(head_out, gate_row, latent, out_weight)


def solution(mesh):
    placed = (
        P("sp", None),
        P("sp", None),
        P("sp"),
        P("sp"),
        P("sp", "tp"),
        P("sp", "tp"),
        P("sp", "tp"),
        P(),
        P(None, "tp"),
        P(None, "tp"),
        P(None, "tp"),
        P(),
        P(),
        P(),
        P(),
        P(),
        P(),
        P(None, "tp"),
    )
    return jax.shard_map(body, mesh=mesh, in_specs=placed, out_specs=P("sp", "tp"), check_vma=False)
```

```python
import functools

import jax
import jax.numpy as jnp
from jax import lax
from jax.experimental import pallas as pl
from jax.experimental.pallas import tpu as pltpu
from jax.sharding import PartitionSpec as P

HEAD_DIM = 128
CHUNK = 128
epsilon = 0.0001
bf16 = jnp.bfloat16
f32 = jnp.float32


def mm(a, b):
    return jnp.dot(a.astype(bf16), b.astype(bf16), preferred_element_type=f32)


def spans(tokens, ctx_tokens):
    size = min(CHUNK, tokens)
    lat = [(at, size) for at in range(0, tokens, size)]
    ctx_size = min(CHUNK, ctx_tokens)
    ctx = [(tokens + at, ctx_size) for at in range(0, ctx_tokens, ctx_size)]
    return lat, ctx


def prep_kernel(tokens, ctx_tokens, q_ref, k_ref, v_ref, col_ref, row_ref, o_ref, e_ref, map_ref):
    lat, ctx = spans(tokens, ctx_tokens)
    items = []
    shared = {}
    for at, size in lat + ctx:
        keys = k_ref[at : at + size, :]
        keys_t = keys.astype(f32).T
        gram = jnp.dot(keys, keys_t.astype(bf16), preferred_element_type=f32)
        rows = lax.broadcasted_iota(jnp.int32, (size, size), 0)
        cols = lax.broadcasted_iota(jnp.int32, (size, size), 1)
        diag = jnp.where(rows == cols, gram, 0.0)
        s_col = lax.rsqrt(jnp.sum(diag, axis=1, keepdims=True) + epsilon)
        s_row = lax.rsqrt(jnp.sum(diag, axis=0, keepdims=True) + epsilon)
        gram = gram * s_col * s_row
        entry = dict(keys=keys.astype(f32) * s_col, keys_t=keys_t * s_row, values=v_ref[at : at + size, :].astype(f32))
        if at < tokens:
            queries = q_ref[at : at + size, :].astype(f32)
            q_scale = lax.rsqrt(jnp.sum(queries * queries, axis=1, keepdims=True) + epsilon) * HEAD_DIM**-0.5
            entry["queries"] = queries * q_scale
            entry["score"] = (
                jnp.dot(q_ref[at : at + size, :], keys_t.astype(bf16), preferred_element_type=f32) * q_scale * s_row
            )
        shared[at] = entry
        for d in range(2):
            rate_col = col_ref[0, at : at + size, 2 * d : 2 * d + 1]
            run_col = col_ref[0, at : at + size, 2 * d + 1 : 2 * d + 2]
            run_row = row_ref[0, 2 * d + 1 : 2 * d + 2, at : at + size]
            inside = rows >= cols if d == 0 else rows <= cols
            strict = rows > cols if d == 0 else rows < cols
            decay = jnp.where(inside, jnp.exp(jnp.minimum(run_col - run_row, 0.0)), 0.0)
            system = jnp.where(strict, gram * decay * rate_col, 0.0)
            item = dict(at=at, size=size, d=d, rate_col=rate_col, run_col=run_col, run_row=run_row)
            item["system"] = system
            if at < tokens:
                item["score"] = entry["score"] * decay
            near = (rows // 2) == (cols // 2)
            item["inv"] = jnp.where(rows == cols, 1.0, jnp.where(near, -system, 0.0))
            items.append(item)
    span = 2
    while span < max(item["size"] for item in items):
        firsts = []
        for item in items:
            if span >= item["size"]:
                firsts.append(None)
                continue
            size = item["size"]
            rows = lax.broadcasted_iota(jnp.int32, (size, size), 0) // span
            cols = lax.broadcasted_iota(jnp.int32, (size, size), 1) // span
            if item["d"] == 0:
                mask = ((rows % 2) == 1) & (cols == rows - 1)
            else:
                mask = ((cols % 2) == 1) & (rows == cols - 1)
            firsts.append(mm(jnp.where(mask, item["system"], 0.0), item["inv"]))
        for item, first in zip(items, firsts):
            if first is not None:
                item["inv"] = item["inv"] - mm(item["inv"], first)
        span *= 2
    for item in items:
        entry = shared[item["at"]]
        growth = jnp.exp(item["run_col"])
        both = jnp.concatenate(
            [entry["values"] * item["rate_col"], entry["keys"] * (item["rate_col"] * growth)], axis=1
        )
        item["solved"] = mm(item["inv"], both)
        last = item["run_row"][:, item["size"] - 1 :] if item["d"] == 0 else item["run_row"][:, :1]
        item["gate"] = jnp.exp(last)
        late_t = entry["keys_t"] * jnp.exp(last - item["run_row"])
        item["late"] = mm(late_t, item["solved"])
        if item["at"] < tokens:
            weighed = mm(item["score"], item["solved"])
            item["local"] = weighed[:, :HEAD_DIM]
            item["early"] = entry["queries"] * growth - weighed[:, HEAD_DIM:]
    eye_r = lax.broadcasted_iota(jnp.int32, (HEAD_DIM, HEAD_DIM), 0)
    eye_c = lax.broadcasted_iota(jnp.int32, (HEAD_DIM, HEAD_DIM), 1)
    eye = (eye_r == eye_c).astype(f32)

    def chain(chunks, d, emit):
        carry = None
        for item in chunks if d == 0 else chunks[::-1]:
            if emit:
                if carry is None:
                    out, early = item["local"], item["early"]
                else:
                    moved = mm(item["early"], carry)
                    out = item["local"] + moved[:, :HEAD_DIM]
                    early = item["early"] + moved[:, HEAD_DIM:]
                e_ref[0, item["at"] : item["at"] + item["size"], d * HEAD_DIM : (d + 1) * HEAD_DIM] = early.astype(
                    bf16
                )
                item["out"] = out
            late, gate = item["late"], item["gate"]
            fresh = jnp.concatenate([late[:, :HEAD_DIM], (gate - 1.0) * eye - late[:, HEAD_DIM:]], axis=1)
            if carry is None:
                carry = fresh
            else:
                carry = gate * carry + fresh - mm(late[:, HEAD_DIM:], carry)
        return carry

    for d in range(2):
        latents = [i for i in items if i["d"] == d and i["at"] < tokens]
        contexts = [i for i in items if i["d"] == d and i["at"] >= tokens]
        map_ref[0, d] = chain(contexts, d, False).astype(bf16)
        map_ref[1, d] = chain(latents, d, True).astype(bf16)
    for at, size in lat:
        pair = [i for i in items if i["at"] == at]
        o_ref[0, at : at + size, :] = pair[0]["out"] + pair[1]["out"]


def apply_maps(maps, state):
    high = state.astype(bf16)
    low = (state - high.astype(f32)).astype(bf16)
    move = maps[:, HEAD_DIM:]
    return (
        state
        + maps[:, :HEAD_DIM].astype(f32)
        + jnp.dot(move, high, preferred_element_type=f32)
        + jnp.dot(move, low, preferred_element_type=f32)
    )


def on_mesh(sp=None, tp=None):
    return (lax.axis_index("sp") if sp is None else sp, lax.axis_index("tp") if tp is None else tp)


def send(src, dst, send_sem, recv_sem, device):
    return pltpu.make_async_remote_copy(
        src_ref=src,
        dst_ref=dst,
        send_sem=send_sem,
        recv_sem=recv_sem,
        device_id=device,
        device_id_type=pl.DeviceIdType.MESH,
    )


def greet(devices):
    barrier = pltpu.get_barrier_semaphore()
    for device in devices:
        pl.semaphore_signal(barrier, inc=1, device_id=device, device_id_type=pl.DeviceIdType.MESH)


def modulation_kernel(
    sp, tp, silu_ref, shift_ref, scale_ref, gate_ref, rows_ref, gate_out, got, blocks, sent_a, recv_a, sent_b, recv_b
):
    me, col = lax.axis_index("sp"), lax.axis_index("tp")
    width = shift_ref.shape[1]
    rings = [on_mesh(sp=lax.rem(me + r, sp)) for r in range(1, sp)]
    cross = [on_mesh(tp=lax.rem(col + r, tp)) for r in range(1, tp)]
    greet(rings + cross)
    silu = silu_ref[...]
    shift = jnp.dot(silu, shift_ref[...], preferred_element_type=f32)
    scale = jnp.dot(silu, scale_ref[...], preferred_element_type=f32)
    gate = jnp.dot(silu, gate_ref[...], preferred_element_type=f32)
    got[me] = jnp.concatenate([shift[0:2], scale[0:2], gate[0:1], jnp.zeros((3, width), f32)], axis=0)
    pl.semaphore_wait(pltpu.get_barrier_semaphore(), len(rings) + len(cross))
    out = []
    for r, device in enumerate(rings):
        out.append(send(got.at[me], got.at[me], sent_a.at[r], recv_a.at[me], device))
        out[-1].start()
    for r in range(1, sp):
        src = lax.rem(me + r, sp)
        send(got.at[src], got.at[src], sent_a.at[0], recv_a.at[src], on_mesh(sp=src)).wait_recv()
    total = got[0]
    for place in range(1, sp):
        total = total + got[place]
    blocks[col] = total
    gate_out[...] = total[4:5]
    for r, device in enumerate(cross):
        out.append(send(blocks.at[col], blocks.at[col], sent_b.at[r], recv_b.at[col], device))
        out[-1].start()
    for r in range(1, tp):
        src = lax.rem(col + r, tp)
        send(blocks.at[src], blocks.at[src], sent_b.at[0], recv_b.at[src], on_mesh(tp=src)).wait_recv()
    for place in range(tp):
        rows_ref[:, place * width : (place + 1) * width] = blocks[place][0:4]
    for copy in out:
        copy.wait_send()


def modulation(silu_rows, shift_weight, scale_weight, gate_weight):
    sp, tp = lax.axis_size("sp"), lax.axis_size("tp")
    width = shift_weight.shape[1]
    vmem = pl.BlockSpec(memory_space=pltpu.VMEM)
    return pl.pallas_call(
        functools.partial(modulation_kernel, sp, tp),
        in_specs=[vmem] * 4,
        out_specs=[vmem] * 2,
        out_shape=[jax.ShapeDtypeStruct((4, tp * width), f32), jax.ShapeDtypeStruct((1, width), f32)],
        scratch_shapes=[
            pltpu.VMEM((sp, 8, width), f32),
            pltpu.VMEM((tp, 8, width), f32),
            pltpu.SemaphoreType.DMA((sp,)),
            pltpu.SemaphoreType.DMA((sp,)),
            pltpu.SemaphoreType.DMA((tp,)),
            pltpu.SemaphoreType.DMA((tp,)),
        ],
        compiler_params=pltpu.CompilerParams(collective_id=0, has_side_effects=True),
        name="modulation",
    )(jnp.pad(silu_rows, ((0, 6), (0, 0))), shift_weight, scale_weight, gate_weight)


def exchange_kernel(
    sp, per, tokens, ctx_tokens, q_ref, k_ref, v_ref, col_ref, row_ref, gain_ref, out_ref,
    o_ref, e_ref, maps_ref, got, starts, back, sent_a, recv_a, sent_b, recv_b,
):
    me = lax.axis_index("sp")
    heads = col_ref.shape[0]
    items = 2 * heads
    peers = [lax.rem(me + r, sp) for r in range(1, sp)]
    greet([on_mesh(sp=peer) for peer in peers])
    pl.semaphore_wait(pltpu.get_barrier_semaphore(), sp - 1)

    def ship(part, item):
        owner, slot = item // per, lax.rem(item, per)
        return owner, send(
            maps_ref.at[part, item],
            got.at[part, me, slot],
            sent_a.at[part, item],
            recv_a.at[part, me, slot],
            on_mesh(sp=owner),
        )

    def one_head(k, unused):
        head = lax.rem(me * per // 2 + heads // 2 + k + (heads - heads // 2 + 1), heads)
        lanes = pl.ds(pl.multiple_of(head * HEAD_DIM, HEAD_DIM), HEAD_DIM)
        prep_kernel(
            tokens,
            ctx_tokens,
            q_ref.at[:, lanes],
            k_ref.at[:, lanes],
            v_ref.at[:, lanes],
            col_ref.at[pl.ds(head, 1)],
            row_ref.at[pl.ds(head, 1)],
            o_ref.at[pl.ds(head, 1)],
            e_ref.at[pl.ds(head, 1)],
            maps_ref.at[:, pl.ds(2 * head, 2)],
        )
        for d in range(2):
            for part in range(2):
                owner, copy = ship(part, 2 * head + d)

                @pl.when(owner != me)
                def _():
                    copy.start()

                @pl.when(owner == me)
                def _():
                    got[part, me, lax.rem(2 * head + d, per)] = maps_ref[part, 2 * head + d]

        return unused

    lax.fori_loop(0, heads, one_head, 0)

    def arrive(part, slot):
        for peer in peers:
            spot = got.at[part, peer, slot]
            send(spot, spot, sent_a.at[part, 0], recv_a.at[part, peer, slot], on_mesh(sp=peer)).wait_recv()

    def give_back(place, slot):
        return send(
            starts.at[place, slot],
            back.at[me, slot],
            sent_b.at[place, slot],
            recv_b.at[me, slot],
            on_mesh(sp=place),
        )

    for slot in range(per):

        @pl.when(me * per + slot < items)
        def _():
            reverse = lax.rem(me * per + slot, 2)
            arrive(0, slot)
            state = jnp.zeros((HEAD_DIM, HEAD_DIM), f32)
            for step in range(sp):
                state = apply_maps(got[0, step + reverse * (sp - 1 - 2 * step), slot], state)
            arrive(1, slot)
            for step in range(sp):
                place = step + reverse * (sp - 1 - 2 * step)
                starts[place, slot] = state.astype(bf16)

                @pl.when(place != me)
                def _():
                    give_back(place, slot).start()

                @pl.when(place == me)
                def _():
                    back[me, slot] = starts[me, slot]

                if step < sp - 1:
                    state = apply_maps(got[1, place, slot], state)

    for item in range(items):
        owner, slot = item // per, item % per

        @pl.when(owner != me)
        def _():
            spot = back.at[owner, slot]
            send(spot, spot, sent_b.at[owner, slot], recv_b.at[owner, slot], on_mesh(sp=owner)).wait_recv()

    for head in range(heads):
        pair = [back[item // per, item % per] for item in (2 * head, 2 * head + 1)]
        combined = o_ref[head] + jnp.dot(
            e_ref[head], jnp.concatenate(pair, axis=0), preferred_element_type=f32
        )
        scale = lax.rsqrt(jnp.mean(combined * combined, axis=1, keepdims=True) + epsilon)
        out_ref[:, head * HEAD_DIM : (head + 1) * HEAD_DIM] = (combined * scale * gain_ref[...]).astype(bf16)
    for item in range(items):
        for part in range(2):
            owner, copy = ship(part, item)

            @pl.when(owner != me)
            def _():
                copy.wait_send()

    for slot in range(per):

        @pl.when(me * per + slot < items)
        def _():
            for peer in peers:
                give_back(peer, slot).wait_send()


def exchange(queries, keys, values, col, row, gain, tokens, ctx_tokens):
    heads = col.shape[0]
    items = 2 * heads
    sp = lax.axis_size("sp")
    per = -(-items // sp)
    vmem = pl.BlockSpec(memory_space=pltpu.VMEM)
    dma = pltpu.SemaphoreType.DMA
    return pl.pallas_call(
        functools.partial(exchange_kernel, sp, per, tokens, ctx_tokens),
        in_specs=[vmem] * 6,
        out_specs=vmem,
        out_shape=jax.ShapeDtypeStruct((tokens, heads * HEAD_DIM), bf16),
        scratch_shapes=[
            pltpu.VMEM((heads, tokens, HEAD_DIM), f32),
            pltpu.VMEM((heads, tokens, 2 * HEAD_DIM), bf16),
            pltpu.VMEM((2, items, HEAD_DIM, 2 * HEAD_DIM), bf16),
            pltpu.VMEM((2, sp, per, HEAD_DIM, 2 * HEAD_DIM), bf16),
            pltpu.VMEM((sp, per, HEAD_DIM, HEAD_DIM), bf16),
            pltpu.VMEM((sp, per, HEAD_DIM, HEAD_DIM), bf16),
            dma((2, items)),
            dma((2, sp, per)),
            dma((sp, per)),
            dma((sp, per)),
        ],
        compiler_params=pltpu.CompilerParams(
            collective_id=1, has_side_effects=True, vmem_limit_bytes=48 * 1024 * 1024
        ),
        name="exchange",
    )(queries, keys, values, col, row, gain)


def output_kernel(
    tp, pieces, head_ref, gate_ref, latent_ref, weight_ref, out_ref,
    got, weight, residual, acc, local_sems, sent_y, recv_y, sent_c, recv_c, sent_r, recv_r,
):
    me, col = lax.axis_index("sp"), lax.axis_index("tp")
    core = lax.rem(col, 2)
    partner = col + 1 - 2 * core
    chips = tp // 2
    far = [lax.rem(col + 2 * r, tp) for r in range(1, chips)]
    far_partner = [place + 1 - 2 * core for place in far]
    tokens, depth = head_ref.shape
    width = out_ref.shape[1]
    rows = tokens // pieces
    load = pltpu.make_async_copy(weight_ref, weight, local_sems.at[0])
    load.start()
    take = pltpu.make_async_copy(
        latent_ref.at[:, pl.ds(pl.multiple_of(col * width, width), width)], residual, local_sems.at[1]
    )
    take.start()
    greet([on_mesh(tp=place) for place in [partner] + far])
    pl.semaphore_wait(pltpu.get_barrier_semaphore(), chips)
    out = []

    def piece(ref, p):
        return ref.at[pl.ds(p * rows, rows)]

    for p in range(pieces):
        for r, place in enumerate(far):
            out.append(
                send(piece(head_ref, p), piece(got.at[col], p), sent_y.at[r, p], recv_y.at[col, p], on_mesh(tp=place))
            )
            out[-1].start()
    for p in range(pieces):
        out.append(
            send(piece(head_ref, p), piece(got.at[col], p), sent_c.at[p], recv_c.at[p], on_mesh(tp=partner))
        )
        out[-1].start()
    load.wait()

    def weights(src):
        return weight[pl.ds(pl.multiple_of(src * depth, depth), depth), :]

    def add(p, block, src, first=False):
        part = jnp.dot(block, weights(src), preferred_element_type=f32)
        at = pl.ds(p * rows, rows)
        acc[at, :] = part if first else acc[at, :] + part

    for p in range(pieces):
        add(p, head_ref[pl.ds(p * rows, rows), :], col, True)
    for p in range(pieces):
        spot = piece(got.at[partner], p)
        send(spot, spot, sent_c.at[p], recv_c.at[p], on_mesh(tp=partner)).wait_recv()
        add(p, spot[...], partner)
    take.wait()
    for p in range(pieces):
        for r, src in enumerate(far):
            spot = piece(got.at[src], p)
            send(spot, spot, sent_y.at[r, p], recv_y.at[src, p], on_mesh(tp=src)).wait_recv()
            out.append(send(spot, spot, sent_r.at[r, p], recv_r.at[src, p], on_mesh(tp=partner)))
            out[-1].start()
            add(p, spot[...], src)
        for r, src in enumerate(far_partner):
            spot = piece(got.at[src], p)
            send(spot, spot, sent_r.at[r, p], recv_r.at[src, p], on_mesh(tp=partner)).wait_recv()
            add(p, spot[...], src)
        at = pl.ds(p * rows, rows)
        out_ref[at, :] = (residual[at, :].astype(f32) + gate_ref[...] * acc[at, :]).astype(bf16)
    for copy in out:
        copy.wait_send()


def output(head_out, gate_row, latent, out_weight):
    tp = lax.axis_size("tp")
    tokens, depth = head_out.shape
    width = out_weight.shape[1]
    pieces = 4
    vmem = pl.BlockSpec(memory_space=pltpu.VMEM)
    anywhere = pl.BlockSpec(memory_space=pl.ANY)
    dma = pltpu.SemaphoreType.DMA
    return pl.pallas_call(
        functools.partial(output_kernel, tp, pieces),
        in_specs=[vmem, vmem, anywhere, anywhere],
        out_specs=vmem,
        out_shape=jax.ShapeDtypeStruct((tokens, width), bf16),
        scratch_shapes=[
            pltpu.VMEM((tp, tokens, depth), bf16),
            pltpu.VMEM(out_weight.shape, bf16),
            pltpu.VMEM((tokens, width), bf16),
            pltpu.VMEM((tokens, width), f32),
            dma((2,)),
            dma((tp, pieces)),
            dma((tp, pieces)),
            dma((pieces,)),
            dma((pieces,)),
            dma((tp, pieces)),
            dma((tp, pieces)),
        ],
        compiler_params=pltpu.CompilerParams(
            collective_id=2, has_side_effects=True, vmem_limit_bytes=63 * 1024 * 1024
        ),
        name="output",
    )(head_out, gate_row, latent, out_weight)


def rms_rows(row_data, row_gain):
    values = row_data.astype(f32)
    scaled = values * lax.rsqrt(jnp.mean(values * values, axis=-1, keepdims=True) + epsilon)
    return scaled * row_gain


def project(matrix, weight):
    return jnp.dot(matrix, weight, preferred_element_type=f32).astype(bf16)


def running_sums(log_decay, size):
    parts = log_decay.reshape((-1, size) + log_decay.shape[1:])
    lower = jnp.tril(jnp.ones((size, size), f32))
    ahead = jnp.einsum("ij,njh->nih", lower, parts[:, :, 0], precision=lax.Precision.HIGHEST)
    behind = jnp.einsum("ji,njh->nih", lower, parts[:, :, 1], precision=lax.Precision.HIGHEST)
    return jnp.stack([ahead, behind], axis=2).reshape(log_decay.shape)


def body(
    latent,
    context,
    condition,
    context_condition,
    shift_weight,
    scale_weight,
    gate_weight,
    norm_gain,
    query_weight,
    key_weight,
    value_weight,
    write_weight,
    decay_weight,
    write_bias,
    decay_bias,
    log_rate,
    head_gain,
    out_weight,
):
    heads_here = query_weight.shape[1] // HEAD_DIM
    first_head = lax.axis_index("tp") * heads_here
    tokens, ctx_tokens = latent.shape[0], context.shape[0]
    stacked = jnp.stack([condition, context_condition]).astype(f32)
    silu_rows = jax.nn.silu(stacked).astype(bf16)
    rows, gate_row = modulation(silu_rows, shift_weight, scale_weight, gate_weight)

    def modulate(row_data, row_index):
        normed = rms_rows(row_data, norm_gain)
        return (normed * (1.0 + rows[2 + row_index]) + rows[row_index]).astype(bf16)

    modulated = jnp.concatenate([modulate(latent, 0), modulate(context, 1)], axis=0)

    def own_heads(array):
        return lax.dynamic_slice_in_dim(array, first_head, heads_here, array.ndim - 1)

    gate_weights = jnp.concatenate(
        [
            own_heads(write_weight).reshape(write_weight.shape[0], -1),
            own_heads(decay_weight).reshape(decay_weight.shape[0], -1),
        ],
        axis=1,
    )
    queries = project(modulated, query_weight)
    keys = project(modulated, key_weight)
    values = project(modulated, value_weight)
    pre = project(modulated, gate_weights).astype(f32).reshape(-1, 2, 2, heads_here)
    rate = jax.nn.sigmoid(pre[:, 0] + own_heads(write_bias))
    log_decay = -jnp.exp(own_heads(log_rate)) * jax.nn.softplus(pre[:, 1] + own_heads(decay_bias))
    lat, ctx = spans(tokens, ctx_tokens)
    running = jnp.concatenate(
        [running_sums(log_decay[:tokens], lat[0][1]), running_sums(log_decay[tokens:], ctx[0][1])], axis=0
    )
    gates = jnp.stack([rate, running], axis=2)
    col = jnp.transpose(gates, (3, 0, 1, 2)).reshape(heads_here, tokens + ctx_tokens, 4)
    row = jnp.transpose(gates, (3, 1, 2, 0)).reshape(heads_here, 4, tokens + ctx_tokens)
    head_out = exchange(queries, keys, values, col, row, head_gain[None, :], tokens, ctx_tokens)
    return output(head_out, gate_row, latent, out_weight)


def solution(mesh):
    placed = (
        P("sp", None),
        P("sp", None),
        P("sp"),
        P("sp"),
        P("sp", "tp"),
        P("sp", "tp"),
        P("sp", "tp"),
        P(),
        P(None, "tp"),
        P(None, "tp"),
        P(None, "tp"),
        P(),
        P(),
        P(),
        P(),
        P(),
        P(),
        P(None, "tp"),
    )
    return jax.shard_map(body, mesh=mesh, in_specs=placed, out_specs=P("sp", "tp"), check_vma=False)
```
